32 devices in a mesh: sp: 8 (over z, x), tp: 4 (over y, core).
Axes of the slice: x: 2, y: 2, z: 4, core: 2. Of those that a mesh axis runs over, the one named last changes fastest.
Arguments:
- probe_vectors: bfloat16 [1024, 2048], P('sp', 'tp'), may hold values from -6 to 6
- address_vectors: bfloat16 [1024, 2048], P('sp', 'tp'), may hold values from -6 to 6
- content_vectors: bfloat16 [1024, 2048], P('sp', 'tp'), may hold values from -6 to 6
- storage_raw_signal: float32 [16, 1024], P('tp', 'sp'), may hold values from -8 to 4
- fade_raw_signal: float32 [16, 1024], P('tp', 'sp'), may hold values from -6 to 6
- channel_fade_exponent: float32 [16], P('tp'), may hold values from -9 to 0
- extra_fade_amount: float32 [16, 1024], P('tp', 'sp'), may hold values from -1 to 0
- sequence_label: int32 [1024], P('sp'), may hold values from 0 to 2, never falling along the last dimension, each value on 1 to 768 neighbouring positions
- exit_valve_raw_signal: bfloat16 [1024, 2048], P('sp', 'tp'), may hold values from -6 to 6
- final_projection_matrix: bfloat16 [2048, 2048], P('tp'), may hold values from -0.125 to 0.125
- incoming_rows_matrix: bfloat16 [1024, 2048], P('sp', 'tp'), may hold values from -48 to 48
- initial_rescale_factor: float32 [2048], P('tp'), may hold values from 0 to 3
- specialist_picks: int32 [1024, 2], P('sp'), may hold values from 0 to 7, all different within a row; in each aligned block of 128 rows (0 to 127, 128 to 255, ...) at most 36 rows name the same one
- picked_specialist_share: bfloat16 [1024, 2], P('sp'), may hold values from 0.29882812 to 1.1953125
- specialist_valve_matrix: bfloat16 [8, 2048, 4096], P('sp', None, 'tp'), may hold values from -0.125 to 0.125
- specialist_raising_matrix: bfloat16 [8, 2048, 4096], P('sp', None, 'tp'), may hold values from -0.125 to 0.125
- specialist_lowering_matrix: bfloat16 [8, 4096, 2048], P('sp', 'tp'), may hold values from -0.09375 to 0.09375
- common_valve_matrix: bfloat16 [2048, 512], P(None, 'tp'), may hold values from -0.125 to 0.125
- common_raising_matrix: bfloat16 [2048, 512], P(None, 'tp'), may hold values from -0.125 to 0.125
- common_lowering_matrix: bfloat16 [512, 2048], P('tp'), may hold values from -0.25 to 0.25
- latter_rescale_factor: float32 [2048], P('tp'), may hold values from 0.1 to 1.9
Outputs:
- result: bfloat16 [1024, 2048], P('sp', 'tp')
The draws below stay inside these ranges and needn't reach their ends.
Inputs may be any that keep to these rules, and one draw needn't show every extreme that they name: `sequence_label`: document numbers never fall; a document has 1 to 768 positions, one exactly 768. `specialist_picks`: each row names 2 different experts; among the rows of one index of sp no expert is named more than 36 times, a bound that some block reaches.
All inputs are finite; a program needn't handle non-finite values.
Results may differ from the reference program's by a relative error of at most 0.018.
Values may be sent and summed in bfloat16 or wider, within the bound.
A program may use at most 64 MiB of HBM per device.

```python
import math
import jax
import jax.numpy as jnp
import numpy as np
from jax import lax

D = 2048
H = 16
DK = 128
DV = 128
BLOCK = 64
FF = 4096
SF = 512
TOP = 2
TOK_DEV = 128
TOKENS = 1024
EXPERTS = 8
CAP = 36
DOC_SPAN = 768
DOCS = 3
N_SP = 8
N_TP = 4


def slow_heads(key):
    share = 0.5
    return jax.random.bernoulli(jax.random.fold_in(key, 11), share, (H,))


def draw_channel_fade_exponent(key, part):
    slower = slow_heads(key)
    jitter = jax.random.uniform(jax.random.fold_in(key, 12), (H,), jnp.float32, -0.3, 0.3)
    slow_rate = math.log(0.6 / DOC_SPAN)
    fast_rate = math.log(2.0 / BLOCK)
    return jnp.where(slower, slow_rate, fast_rate) + jitter


def draw_storage_raw_signal(key, part):
    slower = slow_heads(key)
    base_level = jnp.where(slower, math.log(0.3 * DK / DOC_SPAN), 0.0)
    noise = jnp.clip(jax.random.normal(jax.random.fold_in(key, 13), (H, TOKENS), jnp.float32), -4.0, 4.0)
    return base_level[:, None] + noise


def draw_fade_raw_signal(key, part):
    offsets = jax.random.uniform(jax.random.fold_in(key, 14), (TOKENS // TOK_DEV,), jnp.float32, -1.2, 1.2)
    spread_out = jnp.repeat(offsets, TOK_DEV)
    noise = jnp.clip(jax.random.normal(jax.random.fold_in(key, 15), (H, TOKENS), jnp.float32), -4.0, 4.0)
    return noise + spread_out[None, :]


def draw_extra_fade_amount(key, part):
    places = jax.random.randint(jax.random.fold_in(key, 16), (H, 12), 0, TOKENS)
    depths = jax.random.uniform(jax.random.fold_in(key, 17), (H, 12), jnp.float32, math.log(0.5), math.log(0.6))
    positions = jnp.arange(TOKENS, dtype=jnp.int32)
    hits = (positions[None, None, :] == places[:, :, None]).astype(jnp.float32)
    return jnp.min(hits * depths[:, :, None], 1)


def draw_incoming_rows_matrix(key, part):
    ramp = jnp.exp(jnp.linspace(math.log(0.5), math.log(1.5), D)) * jax.random.uniform(jax.random.fold_in(key, 18), (D,), jnp.float32, 0.7, 1.3)
    row_scale = jnp.exp(jax.random.uniform(jax.random.fold_in(key, 19), (TOKENS, 1), jnp.float32, 0.0, math.log(4.0)))
    base_draw = jnp.clip(jax.random.normal(jax.random.fold_in(key, 21), (TOKENS, D), jnp.float32), -5.0, 5.0)
    return (base_draw * ramp[None, :] * row_scale).astype(jnp.bfloat16)


def draw_initial_rescale_factor(key, part):
    ramp = jnp.exp(jnp.linspace(math.log(0.6), math.log(1.8), D))
    noise = jax.random.uniform(jax.random.fold_in(key, 22), (D,), jnp.float32, 0.8, 1.2)
    return ramp * noise


def block_levels(rng, extent, pieces, smallest, top_value):
    level = 1.0
    for dim, shards_of in pieces:
        draws = jax.random.uniform(jax.random.fold_in(jax.random.fold_in(rng, 6), dim), (shards_of,), jnp.float32, smallest / len(pieces), top_value / len(pieces))
        level = level * jnp.repeat(jnp.exp(draws), extent[dim] // shards_of).reshape((-1,) + (1,) * (len(extent) - 1 - dim))
    return level


def length_profile(number_of, total, limit, skew):
    portions = [(1 << 20) // math.isqrt(grade ** skew) + 1 for grade in range(2, number_of + 1)]
    spare, counts = total - limit - (number_of - 1), [1] * (number_of - 1)
    while spare > 0:
        candidates = [i for i in range(number_of - 1) if counts[i] < limit]
        whole, left = sum([portions[i] for i in candidates]), spare
        for i in candidates:
            extra = min(limit - counts[i], max(1, left * portions[i] // whole), spare)
            counts[i] = counts[i] + extra
            spare = spare - extra
    return np.array([limit] + counts)


def uneven(own_key, amount, total, most, skew):
    if amount == 2:
        one = jax.random.randint(own_key, (), max(1, total - most), min(most, total - 1) + 1)
        return jnp.stack([one, total - one])
    lengths = jnp.asarray(length_profile(amount, total, most, skew), jnp.int32)
    pairs = (amount - 1) // 2
    donor, sink = lengths[1:1 + 2 * pairs:2], lengths[2:2 + 2 * pairs:2]
    room = jnp.minimum(donor - 1, most - sink)
    shifted = jax.random.randint(jax.random.fold_in(own_key, 1), (pairs,), 0, 1 << 20) % (room + 1)
    lengths = lengths.at[1:1 + 2 * pairs:2].set(donor - shifted).at[2:2 + 2 * pairs:2].set(sink + shifted)
    return lengths[jax.random.permutation(jax.random.fold_in(own_key, 2), amount)]


def assign_block(own_key, own, number, rows, count, top, reach, skew):
    sequence = jax.random.permutation(own_key, count)
    packed, usual = load_shares(count, rows * top, reach, skew, True), load_shares(count, rows * top, reach, skew, False)
    places = jnp.arange(count)

    def named(tallies, turn):
        used = int((tallies > 0).sum())
        fixed = max(1, used // 4)
        shifted = fixed + (places - fixed + turn * (used - fixed)) % max(1, count - fixed)
        return jnp.zeros((count,), jnp.int32).at[sequence[jnp.where(places < fixed, places, shifted)]].set(jnp.asarray(tallies, jnp.int32))

    tallies = jnp.where(number % 4 == 0, named(packed, number // 4), named(usual, number - number // 4 - 1))
    mixed = jax.random.permutation(jax.random.fold_in(own, 3), count)
    donor, sink = mixed[0:count // 2 * 2:2], mixed[1:count // 2 * 2:2]
    slack = jnp.minimum(tallies[donor] - 1, reach - tallies[sink]) // 2
    slack = jnp.where((donor == sequence[0]) | (sink == sequence[0]) | (tallies[sink] == 0), 0, jnp.maximum(slack, 0))
    shifted = jax.random.randint(jax.random.fold_in(own, 4), (count // 2,), 0, 1 << 20) % (slack + 1)
    tallies = tallies.at[donor].add(-shifted).at[sink].add(shifted)
    members = jnp.searchsorted(jnp.cumsum(tallies), jnp.arange(rows * top), side="right").astype(jnp.int32)
    table = members.reshape(top, rows).T
    table = table[jax.random.permutation(jax.random.fold_in(own, 1), rows)]
    turn = jax.random.randint(jax.random.fold_in(own, 2), (rows, 1), 0, top)
    return jnp.take_along_axis(table, (jnp.arange(top)[None, :] + turn) % top, axis=1)


def load_shares(count, total, limit, lean, full):
    weights = [(1 << 20) // math.isqrt(grade ** lean) + 1 for grade in range(1, count + 1)]
    largest = limit if full else min(limit, max(-(-total // count), total * weights[0] // sum(weights)))
    least = 1 if total - largest >= count - 1 else 0
    holding, rest = [largest] + [least] * (count - 1), total - largest - least * (count - 1)
    while rest > 0:
        free = [i for i in range(1, count) if holding[i] < largest] or [i for i in range(1, count) if holding[i] < limit]
        pool, remaining = sum([weights[i] for i in free]), rest
        for i in free:
            addition = min(limit - holding[i], max(1, remaining * weights[i] // pool), rest)
            holding[i] = holding[i] + addition
            rest = rest - addition
    return np.array(holding)


def scatter_about(key, shape, width, most, shards=(), kind=jnp.bfloat16):
    drawn = width * jax.random.normal(key, shape, jnp.float32)
    if shards:
        drawn = drawn * block_levels(key, shape, shards, -0.22, 0.18)
    return jnp.clip(drawn, -most, most).astype(kind)


def setup_inputs(seed: int = 0) -> dict:
    splits = jax.random.split(jax.random.key(seed), 22)
    probe_vectors = scatter_about(splits[0], (TOKENS, H * DK), 1.0, 6.0, ((0, 8), (1, 4)))
    address_vectors = scatter_about(splits[1], (TOKENS, H * DK), 1.0, 6.0, ((0, 8), (1, 4)))
    content_vectors = scatter_about(splits[2], (TOKENS, H * DV), 1.0, 6.0, ((0, 8), (1, 4)))
    storage_raw_signal = draw_storage_raw_signal(jax.random.fold_in(splits[21], 71), 0)
    fade_raw_signal = draw_fade_raw_signal(jax.random.fold_in(splits[21], 71), 0)
    channel_fade_exponent = draw_channel_fade_exponent(jax.random.fold_in(splits[21], 71), 0)
    extra_fade_amount = draw_extra_fade_amount(jax.random.fold_in(splits[21], 71), 0)
    sequence_label = jnp.searchsorted(jnp.cumsum(uneven(splits[7], DOCS, TOKENS, DOC_SPAN, 1)), jnp.arange(TOKENS), side="right").astype(jnp.int32)
    exit_valve_raw_signal = scatter_about(splits[8], (TOKENS, H * DV), 1.0, 6.0, ((0, 8), (1, 4)))
    final_projection_matrix = scatter_about(splits[9], (H * DV, D), (H * DV) ** -0.5, 0.125, ((0, 4),))
    incoming_rows_matrix = draw_incoming_rows_matrix(jax.random.fold_in(splits[21], 71), 0)
    initial_rescale_factor = draw_initial_rescale_factor(jax.random.fold_in(splits[21], 71), 0)
    specialist_picks_keys = jax.random.split(jax.random.fold_in(splits[12], 1), TOKENS // TOK_DEV)
    specialist_picks_turns = jax.random.permutation(jax.random.fold_in(splits[12], 3), TOKENS // TOK_DEV)
    specialist_picks = jax.vmap(lambda own, number: assign_block(jax.random.fold_in(splits[12], 2), own, number, TOK_DEV, EXPERTS, TOP, CAP, 1))(specialist_picks_keys, specialist_picks_turns).reshape((TOKENS, TOP))
    picked_specialist_share = jnp.clip(0.29882812 + 0.8964844 * jax.random.uniform(splits[13], (TOKENS, TOP), jnp.float32) ** block_levels(splits[13], (TOKENS, TOP), ((0, 8),), -0.2, 0.2), 0.29882812, 1.1953125).astype(jnp.bfloat16)
    specialist_valve_matrix = scatter_about(splits[14], (EXPERTS, D, FF), D ** -0.5, 0.125, ((0, 8), (2, 4)))
    specialist_raising_matrix = scatter_about(splits[15], (EXPERTS, D, FF), D ** -0.5, 0.125, ((0, 8), (2, 4)))
    specialist_lowering_matrix = scatter_about(splits[16], (EXPERTS, FF, D), FF ** -0.5, 0.09375, ((0, 8), (1, 4)))
    common_valve_matrix = scatter_about(splits[17], (D, SF), D ** -0.5, 0.125, ((1, 4),))
    common_raising_matrix = scatter_about(splits[18], (D, SF), D ** -0.5, 0.125, ((1, 4),))
    common_lowering_matrix = scatter_about(splits[19], (SF, D), SF ** -0.5, 0.25, ((0, 4),))
    latter_rescale_factor = jnp.clip(1.0 + 0.18 * jax.random.normal(splits[20], (D,), jnp.float32), 0.1, 1.9)
    return dict(probe_vectors=probe_vectors, address_vectors=address_vectors, content_vectors=content_vectors, storage_raw_signal=storage_raw_signal, fade_raw_signal=fade_raw_signal, channel_fade_exponent=channel_fade_exponent, extra_fade_amount=extra_fade_amount, sequence_label=sequence_label, exit_valve_raw_signal=exit_valve_raw_signal, final_projection_matrix=final_projection_matrix, incoming_rows_matrix=incoming_rows_matrix, initial_rescale_factor=initial_rescale_factor, specialist_picks=specialist_picks, picked_specialist_share=picked_specialist_share, specialist_valve_matrix=specialist_valve_matrix, specialist_raising_matrix=specialist_raising_matrix, specialist_lowering_matrix=specialist_lowering_matrix, common_valve_matrix=common_valve_matrix, common_raising_matrix=common_raising_matrix, common_lowering_matrix=common_lowering_matrix, latter_rescale_factor=latter_rescale_factor)


HIGH = lax.Precision.HIGHEST
ALPHA = 2.0 ** 0.25

def stored_value(array):
    return lax.optimization_barrier(array.astype(jnp.bfloat16)).astype(jnp.float32)

def unit_rows(array):
    return array * lax.rsqrt(lax.optimization_barrier(jnp.sum(array * array, -1, keepdims=True)) + 1e-06)

def layer_norm(summed, gain):
    row_mean = lax.optimization_barrier(jnp.mean(summed, -1, keepdims=True))
    centred = summed - row_mean
    row_var = lax.optimization_barrier(jnp.mean(centred * centred, -1, keepdims=True))
    return centred * lax.rsqrt(row_var + 1e-05) * gain

def correction_memory_layer(probe_vectors, address_vectors, content_vectors, storage_raw_signal, fade_raw_signal, channel_fade_exponent, extra_fade_amount, sequence_label):
    query_unit = unit_rows(probe_vectors.astype(jnp.float32).reshape(TOKENS, H, DK)) * DK ** (-0.5)
    key_unit = unit_rows(address_vectors.astype(jnp.float32).reshape(TOKENS, H, DK))
    value_rows = content_vectors.astype(jnp.float32).reshape(TOKENS, H, DV)
    write_gate = jax.nn.sigmoid(storage_raw_signal).T
    fade_factor = jnp.exp(extra_fade_amount - jnp.exp(channel_fade_exponent)[:, None] * jax.nn.softplus(fade_raw_signal)).T
    prior = jnp.concatenate([sequence_label[:1], sequence_label[:-1]])
    keep_state = (sequence_label == prior).astype(jnp.float32)

    def advance(carry_state, inputs):
        query_t, key_t, value_t, write_t, decay_t, keep_t = inputs
        carry_state = carry_state * keep_t
        read_back = jnp.einsum('hd,hde->he', key_t, carry_state, precision=HIGH)
        erased = carry_state - write_t[:, None, None] * key_t[:, :, None] * read_back[:, None, :]
        carry_state = decay_t[:, None, None] * erased + write_t[:, None, None] * key_t[:, :, None] * value_t[:, None, :]
        output_t = jnp.einsum('hd,hde->he', query_t, carry_state, precision=HIGH)
        return (carry_state, output_t)
    initial = jnp.zeros((H, DK, DV), jnp.float32)
    unused, memory_layer_result = lax.scan(advance, initial, (query_unit, key_unit, value_rows, write_gate, fade_factor, keep_state))
    return memory_layer_result

def expert_layer(middle, specialist_picks, picked_specialist_share, specialist_valve_matrix, specialist_raising_matrix, specialist_lowering_matrix, common_valve_matrix, common_raising_matrix, common_lowering_matrix):
    picks = TOKENS * TOP
    slots = N_SP * CAP
    flat_routes = specialist_picks.reshape(picks)
    flat_weights = picked_specialist_share.reshape(picks).astype(jnp.float32)
    group_ff = FF // N_TP
    group_sf = SF // N_TP

    def visit(total, expert):
        chosen = flat_routes == expert
        rank_in = jnp.cumsum(chosen.astype(jnp.int32)) - 1
        target = jnp.where(chosen, rank_in, slots)
        owner = jnp.full((slots,), picks, jnp.int32).at[target].set(jnp.arange(picks, dtype=jnp.int32), mode='drop')
        live = (owner < picks).astype(jnp.float32)
        safe_owner = jnp.minimum(owner, picks - 1)
        source_row = safe_owner // TOP
        shared_flag = (safe_owner % TOP == 0).astype(jnp.float32) * live
        weight_e = flat_weights[safe_owner] * live
        inputs_e = middle[source_row]
        gate_e = jnp.dot(inputs_e, specialist_valve_matrix[expert], preferred_element_type=jnp.float32)
        up_e = jnp.dot(inputs_e, specialist_raising_matrix[expert], preferred_element_type=jnp.float32)
        hidden_e = (jax.nn.silu(gate_e) * up_e * weight_e[:, None]).astype(jnp.bfloat16)
        shared_g = jnp.dot(inputs_e, common_valve_matrix, preferred_element_type=jnp.float32)
        shared_u = jnp.dot(inputs_e, common_raising_matrix, preferred_element_type=jnp.float32)
        shared_hidden = (jax.nn.silu(shared_g) * shared_u * shared_flag[:, None]).astype(jnp.bfloat16)
        down_e = specialist_lowering_matrix[expert]
        summed = jnp.zeros((slots, D), jnp.float32)
        for group in range(N_TP):
            term = jnp.dot(hidden_e[:, group * group_ff:(group + 1) * group_ff], down_e[group * group_ff:(group + 1) * group_ff], preferred_element_type=jnp.float32)
            term = term + jnp.dot(shared_hidden[:, group * group_sf:(group + 1) * group_sf], common_lowering_matrix[group * group_sf:(group + 1) * group_sf], preferred_element_type=jnp.float32)
            summed = summed + stored_value(term)
        route_out = stored_value(summed)
        total = total.at[source_row].add(route_out * live[:, None])
        return (total, None)
    start = jnp.zeros((TOKENS, D), jnp.float32)
    mixture, unused = lax.scan(visit, start, jnp.arange(EXPERTS, dtype=jnp.int32))
    return mixture

def reference(probe_vectors, address_vectors, content_vectors, storage_raw_signal, fade_raw_signal, channel_fade_exponent, extra_fade_amount, sequence_label, exit_valve_raw_signal, final_projection_matrix, incoming_rows_matrix, initial_rescale_factor, specialist_picks, picked_specialist_share, specialist_valve_matrix, specialist_raising_matrix, specialist_lowering_matrix, common_valve_matrix, common_raising_matrix, common_lowering_matrix, latter_rescale_factor):
    memory_layer_result = correction_memory_layer(probe_vectors, address_vectors, content_vectors, storage_raw_signal, fade_raw_signal, channel_fade_exponent, extra_fade_amount, sequence_label)
    scaled = memory_layer_result * lax.rsqrt(lax.optimization_barrier(jnp.mean(memory_layer_result * memory_layer_result, -1, keepdims=True)) + 1e-06)
    heads_out = (scaled.reshape(TOKENS, H * DV) * jax.nn.silu(exit_valve_raw_signal.astype(jnp.float32))).astype(jnp.bfloat16)
    group_rows = H * DV // N_TP
    projected = jnp.zeros((TOKENS, D), jnp.float32)
    for group in range(N_TP):
        term = jnp.dot(heads_out[:, group * group_rows:(group + 1) * group_rows], final_projection_matrix[group * group_rows:(group + 1) * group_rows], preferred_element_type=jnp.float32)
        projected = projected + stored_value(term)
    first_sum = ALPHA * incoming_rows_matrix.astype(jnp.float32) + projected
    middle = layer_norm(first_sum, initial_rescale_factor).astype(jnp.bfloat16)
    mixture = expert_layer(middle, specialist_picks, picked_specialist_share, specialist_valve_matrix, specialist_raising_matrix, specialist_lowering_matrix, common_valve_matrix, common_raising_matrix, common_lowering_matrix)
    second_sum = ALPHA * middle.astype(jnp.float32) + mixture
    return layer_norm(second_sum, latter_rescale_factor).astype(jnp.bfloat16)
```

```python
import functools

import jax
import jax.numpy as jnp
from jax import lax
from jax.experimental import pallas as pl
from jax.experimental.pallas import tpu as pltpu
from jax.sharding import PartitionSpec as P

DK = 128
DV = 128
BLOCK = 64
DOC_SPAN = 768


HIGH = lax.Precision.HIGHEST
ALPHA = 2.0**0.25
MESH = pl.DeviceIdType.MESH


def vmem_specs(count):
    return [pl.BlockSpec(memory_space=pltpu.VMEM)] * count


def exchange_kernel(axis, n, modes, *refs):
    count = len(modes)
    ins, outs = refs[:count], refs[count : 2 * count]
    send_sem, recv_sem, own_sem = refs[2 * count :]
    me = lax.axis_index(axis)
    barrier = pltpu.get_barrier_semaphore()
    for hop in range(1, n):
        pl.semaphore_signal(
            barrier, inc=1, device_id={axis: lax.rem(me + hop, n)}, device_id_type=MESH
        )

    def span(ref, place, size):
        return ref.at[:, pl.ds(pl.multiple_of(place * size, size), size)]

    def ends(index, target):
        source, landing = ins[index], outs[index]
        if modes[index] == "rows":
            return source.at[target], landing.at[me]
        if modes[index] == "cols":
            return span(source, target, landing.shape[-1]), landing.at[me]
        if modes[index] == "join":
            return source, span(landing, me, source.shape[-1])
        return source, landing.at[me]

    own = []
    for index in range(count):
        source, landing = ends(index, me)
        own.append(pltpu.make_async_copy(source, landing, own_sem.at[index]))
        own[-1].start()
    pl.semaphore_wait(barrier, n - 1)
    sent = []
    for hop in range(1, n):
        target = lax.rem(me + hop, n)
        for index in range(count):
            source, landing = ends(index, target)
            sent.append(
                pltpu.make_async_remote_copy(
                    src_ref=source,
                    dst_ref=landing,
                    send_sem=send_sem.at[index, hop - 1],
                    recv_sem=recv_sem.at[index, hop - 1],
                    device_id={axis: target},
                    device_id_type=MESH,
                )
            )
            sent[-1].start()
    for copy in own + sent:
        copy.wait()


def exchange(arrays, modes, axis, cid):
    n = lax.axis_size(axis)
    count = len(arrays)
    shapes = []
    for array, mode in zip(arrays, modes):
        if mode == "rows":
            shape = array.shape
        elif mode == "cols":
            shape = (n, array.shape[0], array.shape[1] // n)
        elif mode == "join":
            shape = (array.shape[0], array.shape[1] * n)
        else:
            shape = (n,) + array.shape
        shapes.append(jax.ShapeDtypeStruct(shape, array.dtype))
    return pl.pallas_call(
        functools.partial(exchange_kernel, axis, n, modes),
        out_shape=shapes,
        in_specs=vmem_specs(count),
        out_specs=vmem_specs(count),
        scratch_shapes=[
            pltpu.SemaphoreType.DMA((count, n - 1)),
            pltpu.SemaphoreType.DMA((count, n - 1)),
            pltpu.SemaphoreType.DMA((count,)),
        ],
        compiler_params=pltpu.CompilerParams(collective_id=cid, has_side_effects=True),
        name=f"exchange_{axis}_{cid}",
    )(*arrays)


def scan_plan(n, reach):
    hops = [1]
    covered = 1
    if reach > 1 and n > 2:
        hops.append(2)
        covered = 3
        while covered < min(reach, n - 1):
            hops.append(covered)
            covered = 2 * covered
    return hops


def scan_kernel(n, hops, own_ref, out_ref, *scratch):
    rounds = len(hops)
    landed, built = scratch[:rounds], scratch[rounds : 2 * rounds]
    send_sem, recv_sem = scratch[2 * rounds :]
    heads = own_ref.shape[1]
    me = lax.axis_index("sp")
    barrier = pltpu.get_barrier_semaphore()
    for hop in range(1, n):
        pl.semaphore_signal(
            barrier, inc=1, device_id={"sp": lax.rem(me + hop, n)}, device_id_type=MESH
        )
    pl.semaphore_wait(barrier, n - 1)

    def dot(left, right):
        return jnp.dot(left, right, preferred_element_type=jnp.float32)

    def copy_of(index):
        last = index == rounds - 1 and index > 1
        source = own_ref if index == 0 else built[index]
        landing = landed[index]
        if last:
            source, landing = source.at[1], landing.at[1]
        return pltpu.make_async_remote_copy(
            src_ref=source,
            dst_ref=landing,
            send_sem=send_sem.at[index],
            recv_sem=recv_sem.at[index],
            device_id={"sp": lax.rem(me + hops[index], n)},
            device_id_type=MESH,
        )

    window = None
    for index, hop in enumerate(hops):
        copy = copy_of(index)
        last = index == rounds - 1

        @pl.when(me + hop < n)
        def _():
            copy.start()

        @pl.when(me >= hop)
        def _():
            copy.wait_recv()

        @pl.when(me < hop)
        def _():
            landed[index][...] = jnp.zeros_like(landed[index])

        got = landed[index]
        if index == 0:
            if last:
                out_ref[...] = got[1].astype(jnp.float32)
            else:
                later, target = own_ref, built[1]
                for h in range(heads):
                    target[0, h] = dot(later[0, h], got[0, h]).astype(target.dtype)
                    target[1, h] = (
                        dot(later[0, h], got[1, h]) + later[1, h].astype(jnp.float32)
                    ).astype(target.dtype)
            window = got
        else:
            for h in range(heads):
                shift = dot(window[0, h], got[1, h]) + window[1, h].astype(jnp.float32)
                if last:
                    out_ref[h] = shift
                else:
                    target = built[index + 1]
                    target[0, h] = dot(window[0, h], got[0, h]).astype(target.dtype)
                    target[1, h] = shift.astype(target.dtype)
            if not last:
                window = built[index + 1]
    for index, hop in enumerate(hops):

        @pl.when(me + hop < n)
        def _():
            copy_of(index).wait_send()


def entering(summary, reach, cid):
    n = lax.axis_size("sp")
    hops = scan_plan(n, reach)
    block = pltpu.VMEM(summary.shape, summary.dtype)
    return pl.pallas_call(
        functools.partial(scan_kernel, n, hops),
        out_shape=jax.ShapeDtypeStruct(summary.shape[1:], jnp.float32),
        in_specs=vmem_specs(1),
        out_specs=pl.BlockSpec(memory_space=pltpu.VMEM),
        scratch_shapes=[block] * (2 * len(hops))
        + [pltpu.SemaphoreType.DMA((len(hops),)), pltpu.SemaphoreType.DMA((len(hops),))],
        compiler_params=pltpu.CompilerParams(collective_id=cid, has_side_effects=True),
        name="state_scan",
    )(summary)


def unit_rows(array):
    return array * lax.rsqrt(jnp.sum(array * array, -1, keepdims=True) + 1e-06)


def matmul_high(form, left, right):
    return jnp.einsum(form, left, right, precision=HIGH)


def matmul_one(form, left, right):
    return jnp.einsum(
        form,
        left.astype(jnp.bfloat16),
        right.astype(jnp.bfloat16),
        preferred_element_type=jnp.float32,
    )


def feature_norm(summed, gain, cid):
    width = summed.shape[-1] * lax.axis_size("tp")
    own = jnp.stack([jnp.sum(summed, -1), jnp.sum(summed * summed, -1)])
    (parts,) = exchange((own,), ("all",), "tp", cid)
    totals, squares = jnp.sum(parts, 0)
    row_mean = totals / width
    row_var = squares / width - row_mean * row_mean
    return (summed - row_mean[:, None]) * lax.rsqrt(row_var[:, None] + 1e-05) * gain


def block_pass(query_unit, key_unit, write_gate, decay_logarithm, segment, values_in, initial):
    heads_here, blocks, block_len, key_depth = query_unit.shape
    cumulative = jnp.cumsum(decay_logarithm, -1)
    before = jnp.concatenate([segment[:1, 0], segment[:-1, -1]])
    carried = (segment == before[:, None]).astype(jnp.float32)
    same_doc = segment[:, :, None] == segment[:, None, :]
    offsets = jnp.arange(block_len)
    lower_tri = offsets[:, None] >= offsets[None, :]
    strict = offsets[:, None] > offsets[None, :]
    log_gap = cumulative[..., :, None] - cumulative[..., None, :]
    reach_mask = jnp.where(lower_tri & same_doc, jnp.exp(jnp.where(lower_tri, log_gap, 0.0)), 0.0)
    weighted_keys = key_unit * write_gate[..., None]
    coupling = jnp.where(
        strict, matmul_high("hncd,hnsd->hncs", weighted_keys, key_unit) * reach_mask, 0.0
    )
    identity_block = jnp.eye(block_len, dtype=jnp.float32)
    inverse = identity_block - coupling
    nil_power = coupling
    for squaring in range(block_len.bit_length() - 2):
        nil_power = matmul_high("hncs,hnst->hnct", nil_power, nil_power)
        inverse = matmul_high("hncs,hnst->hnct", inverse, identity_block + nil_power)
    growth = jnp.exp(cumulative) * carried
    update = matmul_one("hncs,hnse->hnce", inverse, values_in * write_gate[..., None])
    correction = matmul_one("hncs,hnsd->hncd", inverse, weighted_keys * growth[..., None])
    final_growth = jnp.exp(cumulative[..., -1]) * (segment[:, -1] == before).astype(jnp.float32)
    tail_decay = jnp.exp(cumulative[..., -1:] - cumulative) * (segment == segment[:, -1:]).astype(
        jnp.float32
    )
    tail_keys = key_unit * tail_decay[..., None]
    query_grown = query_unit * growth[..., None]
    local_scores = matmul_one("hncd,hnsd->hncs", query_unit, key_unit) * reach_mask

    def advance(carry_state, inputs):
        grown_query, block_corr, block_update, block_keys, block_scores, block_fade = inputs
        fresh_values = block_update - matmul_one("hcd,hde->hce", block_corr, carry_state)
        next_state = carry_state * block_fade[:, None, None] + matmul_one(
            "hcd,hce->hde", block_keys, fresh_values
        )
        block_out = matmul_one("hcd,hde->hce", grown_query, carry_state) + matmul_one(
            "hcs,hse->hce", block_scores, fresh_values
        )
        return (next_state, block_out)

    inputs = tuple(
        (
            jnp.moveaxis(array, 1, 0)
            for array in (query_grown, correction, update, tail_keys, local_scores, final_growth)
        )
    )
    final_state, outputs = lax.scan(advance, initial, inputs)
    outputs = jnp.moveaxis(outputs, 0, 1).reshape(heads_here, blocks * block_len, -1)
    return (final_state, outputs)


def shards(
    probe_vectors,
    address_vectors,
    content_vectors,
    storage_raw_signal,
    fade_raw_signal,
    channel_fade_exponent,
    extra_fade_amount,
    sequence_label,
    exit_valve_raw_signal,
    final_projection_matrix,
    incoming_rows_matrix,
    initial_rescale_factor,
    specialist_picks,
    picked_specialist_share,
    specialist_valve_matrix,
    specialist_raising_matrix,
    specialist_lowering_matrix,
    common_valve_matrix,
    common_raising_matrix,
    common_lowering_matrix,
    latter_rescale_factor,
):
    tokens_here = probe_vectors.shape[0]
    heads_here = storage_raw_signal.shape[0]
    blocks = tokens_here // BLOCK

    def split_heads(array, width):
        moved = jnp.transpose(
            array.astype(jnp.float32).reshape(tokens_here, heads_here, width), (1, 0, 2)
        )
        return moved.reshape(heads_here, blocks, BLOCK, width)

    query_unit = unit_rows(split_heads(probe_vectors, DK)) * DK ** (-0.5)
    key_unit = unit_rows(split_heads(address_vectors, DK))
    value_rows = split_heads(content_vectors, DV)
    write_gate = jax.nn.sigmoid(storage_raw_signal).reshape(heads_here, blocks, BLOCK)
    decay_logarithm = (
        extra_fade_amount
        - jnp.exp(channel_fade_exponent)[:, None] * jax.nn.softplus(fade_raw_signal)
    ).reshape(heads_here, blocks, BLOCK)
    segment = sequence_label.astype(jnp.float32).reshape(blocks, BLOCK)
    extended = jnp.concatenate(
        [value_rows, jnp.zeros((heads_here, blocks, BLOCK, DK), jnp.float32)], -1
    )
    identity_state = jnp.broadcast_to(jnp.eye(DK, dtype=jnp.float32), (heads_here, DK, DK))
    start_state = jnp.concatenate(
        [jnp.zeros((heads_here, DK, DV), jnp.float32), identity_state], -1
    )
    summary, local_out = block_pass(
        query_unit, key_unit, write_gate, decay_logarithm, segment, extended, start_state
    )
    (edges,) = exchange((sequence_label[None, :],), ("all",), "sp", 0)
    place = lax.axis_index("sp")
    before = lax.dynamic_index_in_dim(edges[:, 0, -1], jnp.maximum(place - 1, 0), 0, False)
    joined = ((before == sequence_label[0]) & (place > 0)).astype(jnp.float32)
    reach = -(-(DOC_SPAN - 1) // tokens_here)
    own = jnp.stack([summary[..., DV:] * joined, summary[..., :DV]]).astype(jnp.bfloat16)
    incoming = entering(own, reach, 1) * joined
    memory_layer_result = local_out[..., :DV] + matmul_one(
        "hcd,hde->hce", local_out[..., DV:], incoming
    )
    scaled = memory_layer_result * lax.rsqrt(
        jnp.mean(memory_layer_result * memory_layer_result, -1, keepdims=True) + 1e-06
    )
    token_major = jnp.transpose(scaled, (1, 0, 2)).reshape(tokens_here, heads_here * DV)
    heads_out = (token_major * jax.nn.silu(exit_valve_raw_signal.astype(jnp.float32))).astype(
        jnp.bfloat16
    )
    partial_proj = jnp.dot(heads_out, final_projection_matrix, preferred_element_type=jnp.float32)
    (shares,) = exchange((partial_proj.astype(jnp.bfloat16),), ("cols",), "tp", 2)
    projected = jnp.sum(shares.astype(jnp.float32), 0)
    middle = feature_norm(
        ALPHA * incoming_rows_matrix.astype(jnp.float32) + projected, initial_rescale_factor, 3
    ).astype(jnp.bfloat16)
    top = specialist_picks.shape[1]
    local_experts = specialist_valve_matrix.shape[0]
    experts_all = local_experts * lax.axis_size("sp")
    capacity = max(2, 9 * tokens_here * top // (8 * experts_all))
    picks = tokens_here * top
    flat_routes = specialist_picks.reshape(picks)
    one_hot = (flat_routes[:, None] == jnp.arange(experts_all, dtype=jnp.int32)[None, :]).astype(
        jnp.int32
    )
    rank_in = jnp.sum(jnp.cumsum(one_hot, 0) * one_hot, 1) - 1
    slot_of = flat_routes * capacity + rank_in
    slots = experts_all * capacity
    slot_table = slot_of.reshape(tokens_here, top)
    matches = [
        jnp.arange(slots, dtype=jnp.int32)[:, None] == slot_table[None, :, j] for j in range(top)
    ]
    pick = functools.reduce(jnp.logical_or, matches).astype(jnp.bfloat16)
    slot_weight = sum(
        jnp.sum(
            jnp.where(matches[j], picked_specialist_share[None, :, j].astype(jnp.float32), 0.0), 1
        )
        for j in range(top)
    )
    slot_shared = jnp.any(matches[0], 1).astype(jnp.float32)
    slot_info = jnp.stack([slot_weight, slot_shared]).astype(jnp.bfloat16)
    slot_info = jnp.moveaxis(slot_info.reshape(2, experts_all, capacity), 0, 1)
    sp_size = lax.axis_size("sp")
    slot_count = capacity * local_experts
    sent = jnp.dot(pick, middle, preferred_element_type=jnp.float32).astype(jnp.bfloat16)
    arrived, info = exchange(
        (sent.reshape(sp_size, slot_count, -1), slot_info.reshape(sp_size, local_experts * 2, capacity)),
        ("rows", "rows"),
        "sp",
        5,
    )
    sources = sp_size
    (inputs_e,) = exchange((arrived.reshape(sources * slot_count, -1),), ("join",), "tp", 6)
    info = info.astype(jnp.float32)
    weight_e = info[:, 0].reshape(-1, 1)
    shared_e = info[:, 1].reshape(-1, 1)
    gate_e = jnp.dot(inputs_e, specialist_valve_matrix[0], preferred_element_type=jnp.float32)
    up_e = jnp.dot(inputs_e, specialist_raising_matrix[0], preferred_element_type=jnp.float32)
    hidden_e = (jax.nn.silu(gate_e) * up_e * weight_e).astype(jnp.bfloat16)
    shared_g = jnp.dot(inputs_e, common_valve_matrix, preferred_element_type=jnp.float32)
    shared_u = jnp.dot(inputs_e, common_raising_matrix, preferred_element_type=jnp.float32)
    shared_hidden = (jax.nn.silu(shared_g) * shared_u * shared_e).astype(jnp.bfloat16)
    partial_out = jnp.dot(
        hidden_e, specialist_lowering_matrix[0], preferred_element_type=jnp.float32
    )
    partial_out = partial_out + jnp.dot(
        shared_hidden, common_lowering_matrix, preferred_element_type=jnp.float32
    )
    (pieces,) = exchange((partial_out.astype(jnp.bfloat16),), ("cols",), "tp", 7)
    summed = jnp.sum(pieces.astype(jnp.float32), 0).astype(jnp.bfloat16)
    (returned,) = exchange((summed.reshape(sources, slot_count, -1),), ("rows",), "sp", 8)
    mixture = lax.dot_general(
        pick,
        returned.reshape(slots, -1),
        (((0,), (0,)), ((), ())),
        preferred_element_type=jnp.float32,
    )
    second_sum = ALPHA * middle.astype(jnp.float32) + mixture
    return feature_norm(second_sum, latter_rescale_factor, 4).astype(jnp.bfloat16)


def solution(mesh):
    placed = (
        P("sp", "tp"),
        P("sp", "tp"),
        P("sp", "tp"),
        P("tp", "sp"),
        P("tp", "sp"),
        P("tp"),
        P("tp", "sp"),
        P("sp"),
        P("sp", "tp"),
        P("tp", None),
        P("sp", "tp"),
        P("tp"),
        P("sp", None),
        P("sp", None),
        P("sp", None, "tp"),
        P("sp", None, "tp"),
        P("sp", "tp", None),
        P(None, "tp"),
        P(None, "tp"),
        P("tp", None),
        P("tp"),
    )
    return jax.shard_map(
        shards, mesh=mesh, in_specs=placed, out_specs=P("sp", "tp"), check_vma=False
    )
```

```python
import functools

import jax
import jax.numpy as jnp
from jax import lax
from jax.experimental import pallas as pl
from jax.experimental.pallas import tpu as pltpu
from jax.sharding import PartitionSpec as P

DK = 128
DV = 128
BLOCK = 64
DOC_SPAN = 768


HIGH = lax.Precision.HIGHEST
ALPHA = 2.0**0.25
MESH = pl.DeviceIdType.MESH


def vmem_specs(count):
    return [pl.BlockSpec(memory_space=pltpu.VMEM)] * count


def exchange_kernel(axis, n, modes, *refs):
    count = len(modes)
    ins, outs = refs[:count], refs[count : 2 * count]
    send_sem, recv_sem, own_sem = refs[2 * count :]
    me = lax.axis_index(axis)
    barrier = pltpu.get_barrier_semaphore()
    for hop in range(1, n):
        pl.semaphore_signal(
            barrier, inc=1, device_id={axis: lax.rem(me + hop, n)}, device_id_type=MESH
        )

    def span(ref, place, size):
        return ref.at[:, pl.ds(pl.multiple_of(place * size, size), size)]

    def ends(index, target):
        source, landing = ins[index], outs[index]
        if modes[index] == "rows":
            return source.at[target], landing.at[me]
        if modes[index] == "cols":
            return span(source, target, landing.shape[-1]), landing.at[me]
        if modes[index] == "join":
            return source, span(landing, me, source.shape[-1])
        return source, landing.at[me]

    own = []
    for index in range(count):
        source, landing = ends(index, me)
        own.append(pltpu.make_async_copy(source, landing, own_sem.at[index]))
        own[-1].start()
    pl.semaphore_wait(barrier, n - 1)
    sent = []
    for hop in range(1, n):
        target = lax.rem(me + hop, n)
        for index in range(count):
            source, landing = ends(index, target)
            sent.append(
                pltpu.make_async_remote_copy(
                    src_ref=source,
                    dst_ref=landing,
                    send_sem=send_sem.at[index, hop - 1],
                    recv_sem=recv_sem.at[index, hop - 1],
                    device_id={axis: target},
                    device_id_type=MESH,
                )
            )
            sent[-1].start()
    for copy in own + sent:
        copy.wait()


def exchange(arrays, modes, axis, cid):
    n = lax.axis_size(axis)
    count = len(arrays)
    shapes = []
    for array, mode in zip(arrays, modes):
        if mode == "rows":
            shape = array.shape
        elif mode == "cols":
            shape = (n, array.shape[0], array.shape[1] // n)
        elif mode == "join":
            shape = (array.shape[0], array.shape[1] * n)
        else:
            shape = (n,) + array.shape
        shapes.append(jax.ShapeDtypeStruct(shape, array.dtype))
    return pl.pallas_call(
        functools.partial(exchange_kernel, axis, n, modes),
        out_shape=shapes,
        in_specs=vmem_specs(count),
        out_specs=vmem_specs(count),
        scratch_shapes=[
            pltpu.SemaphoreType.DMA((count, n - 1)),
            pltpu.SemaphoreType.DMA((count, n - 1)),
            pltpu.SemaphoreType.DMA((count,)),
        ],
        compiler_params=pltpu.CompilerParams(collective_id=cid, has_side_effects=True),
        name=f"exchange_{axis}_{cid}",
    )(*arrays)


def scan_plan(n, reach):
    hops = [1]
    covered = 1
    if reach > 1 and n > 2:
        hops.append(2)
        covered = 3
        while covered < min(reach, n - 1):
            hops.append(covered)
            covered = 2 * covered
    return hops


def scan_kernel(n, hops, own_ref, out_ref, *scratch):
    rounds = len(hops)
    landed, built = scratch[:rounds], scratch[rounds : 2 * rounds]
    send_sem, recv_sem = scratch[2 * rounds :]
    heads = own_ref.shape[1]
    me = lax.axis_index("sp")
    barrier = pltpu.get_barrier_semaphore()
    for hop in range(1, n):
        pl.semaphore_signal(
            barrier, inc=1, device_id={"sp": lax.rem(me + hop, n)}, device_id_type=MESH
        )
    pl.semaphore_wait(barrier, n - 1)

    def dot(left, right):
        return jnp.dot(left, right, preferred_element_type=jnp.float32)

    def copy_of(index):
        last = index == rounds - 1 and index > 1
        source = own_ref if index == 0 else built[index]
        landing = landed[index]
        if last:
            source, landing = source.at[1], landing.at[1]
        return pltpu.make_async_remote_copy(
            src_ref=source,
            dst_ref=landing,
            send_sem=send_sem.at[index],
            recv_sem=recv_sem.at[index],
            device_id={"sp": lax.rem(me + hops[index], n)},
            device_id_type=MESH,
        )

    window = None
    for index, hop in enumerate(hops):
        copy = copy_of(index)
        last = index == rounds - 1

        @pl.when(me + hop < n)
        def _():
            copy.start()

        @pl.when(me >= hop)
        def _():
            copy.wait_recv()

        @pl.when(me < hop)
        def _():
            landed[index][...] = jnp.zeros_like(landed[index])

        got = landed[index]
        if index == 0:
            if last:
                out_ref[...] = got[1].astype(jnp.float32)
            else:
                later, target = own_ref, built[1]
                for h in range(heads):
                    target[0, h] = dot(later[0, h], got[0, h]).astype(target.dtype)
                    target[1, h] = (
                        dot(later[0, h], got[1, h]) + later[1, h].astype(jnp.float32)
                    ).astype(target.dtype)
            window = got
        else:
            for h in range(heads):
                shift = dot(window[0, h], got[1, h]) + window[1, h].astype(jnp.float32)
                if last:
                    out_ref[h] = shift
                else:
                    target = built[index + 1]
                    target[0, h] = dot(window[0, h], got[0, h]).astype(target.dtype)
                    target[1, h] = shift.astype(target.dtype)
            if not last:
                window = built[index + 1]
    for index, hop in enumerate(hops):

        @pl.when(me + hop < n)
        def _():
            copy_of(index).wait_send()


def entering(summary, reach, cid):
    n = lax.axis_size("sp")
    hops = scan_plan(n, reach)
    block = pltpu.VMEM(summary.shape, summary.dtype)
    return pl.pallas_call(
        functools.partial(scan_kernel, n, hops),
        out_shape=jax.ShapeDtypeStruct(summary.shape[1:], jnp.float32),
        in_specs=vmem_specs(1),
        out_specs=pl.BlockSpec(memory_space=pltpu.VMEM),
        scratch_shapes=[block] * (2 * len(hops))
        + [pltpu.SemaphoreType.DMA((len(hops),)), pltpu.SemaphoreType.DMA((len(hops),))],
        compiler_params=pltpu.CompilerParams(collective_id=cid, has_side_effects=True),
        name="state_scan",
    )(summary)


def unit_rows(array):
    return array * lax.rsqrt(jnp.sum(array * array, -1, keepdims=True) + 1e-06)


def matmul_high(form, left, right):
    return jnp.einsum(form, left, right, precision=HIGH)


def matmul_one(form, left, right):
    return jnp.einsum(
        form,
        left.astype(jnp.bfloat16),
        right.astype(jnp.bfloat16),
        preferred_element_type=jnp.float32,
    )


def row_stats(array):
    lane = lax.broadcasted_iota(jnp.int32, (array.shape[0], 128), 1)
    total = jnp.sum(array, -1, keepdims=True)
    square = jnp.sum(array * array, -1, keepdims=True)
    return jnp.where(lane == 0, total, jnp.where(lane == 1, square, 0.0)).T[:8]


def columns_of(rows):
    return jnp.concatenate([rows] * (128 // rows.shape[0]), 0).T


def layer_kernel(
    ns, nt, cap, pad, heads_ref, wo_ref, rows_ref, gain_ref, last_gain_ref, pick_ref, pick_t_ref,
    info_ref, wv_hbm, wr_hbm, wd_hbm, cv_hbm, cr_hbm, cd_hbm, out_ref,
    wv_ref, wr_ref, wd_ref, cv_ref, cr_ref, cd_ref, weight_sem,
    head_out, head_in, head_yout, head_yin, head_sem,
    stat_own, stat_in, stat_sem,
    sbuf, gathered, infos, sp_sem, info_sem, y_sem, pair_sem,
    inputs, hidden, shared, side, part_out, part_in, part_yout, part_yin, part_sem,
    back_out, back_in, back_sem, returned,
):
    sp, tp = lax.axis_index("sp"), lax.axis_index("tp")
    chips = nt // 2
    chip, core = tp // 2, lax.rem(tp, 2)
    partner = tp + 1 - 2 * core
    width = out_ref.shape[-1]
    loads = [
        pltpu.make_async_copy(source, target, weight_sem.at[i])
        for i, (source, target) in enumerate(
            (
                (cv_hbm, cv_ref),
                (cr_hbm, cr_ref),
                (wv_hbm.at[0], wv_ref),
                (wr_hbm.at[0], wr_ref),
                (cd_hbm, cd_ref),
                (wd_hbm.at[0], wd_ref),
            )
        )
    ]
    for load in loads:
        load.start()
    barrier = pltpu.get_barrier_semaphore()
    for hop in range(1, ns):
        pl.semaphore_signal(
            barrier, inc=1, device_id={"sp": lax.rem(sp + hop, ns)}, device_id_type=MESH
        )
    for hop in range(1, nt):
        pl.semaphore_signal(
            barrier, inc=1, device_id={"tp": lax.rem(tp + hop, nt)}, device_id_type=MESH
        )
    inputs[...] = jnp.zeros_like(inputs)
    returned[...] = jnp.zeros_like(returned)
    pl.semaphore_wait(barrier, ns - 1 + nt - 1)
    waits = []

    def send(source, target, sems, place, where):
        copy = pltpu.make_async_remote_copy(
            src_ref=source,
            dst_ref=target,
            send_sem=sems.at[(0,) + place],
            recv_sem=sems.at[(1,) + place],
            device_id=where,
            device_id_type=MESH,
        )
        copy.start()
        waits.append(copy)
        return copy

    def dot(left, right):
        return jnp.dot(left, right, preferred_element_type=jnp.float32)

    def sum_over_tp(block, put, take, out, landed, yout, yin, sems):
        order = list(range(1, chips)) + [0]
        pairs = {}
        for k in order:
            put(out, k, block(2 * lax.rem(chip + k, chips) + 1 - core))
            pairs[k] = send(out.at[k], landed.at[k], sems, (k,), {"tp": partner})
        across = []
        for k in order:
            there = 2 * lax.rem(chip + k, chips) + core
            value = block(there)
            pairs[k].wait_recv()
            value = value + take(landed, k)
            if k:
                put(yout, k - 1, value)
                across.append(
                    send(yout.at[k - 1], yin.at[k - 1], sems, (chips + k - 1,), {"tp": there})
                )
        for k, copy in enumerate(across):
            copy.wait_recv()
            value = value + take(yin, k)
        return value

    def normed(summed, gain, index):
        stat_own[index] = row_stats(summed)
        copies = []
        for hop in range(1, nt):
            copies.append(
                send(
                    stat_own.at[index],
                    stat_in.at[index, hop - 1],
                    stat_sem,
                    (index, hop - 1),
                    {"tp": lax.rem(tp + hop, nt)},
                )
            )
        total = stat_own[index]
        for hop in range(1, nt):
            copies[hop - 1].wait_recv()
            total = total + stat_in[index, hop - 1]
        total = columns_of(total / (width * nt))
        mean, square = total[:, 0:1], total[:, 1:2]
        return (summed - mean) * lax.rsqrt(square - mean * mean + 1e-05) * gain

    def head_block(t):
        start = pl.multiple_of(t * width, width)
        return dot(heads_ref[...], wo_ref[:, pl.ds(start, width)])

    def put_plain(ref, k, value):
        ref[k] = value.astype(ref.dtype)

    def take_plain(ref, k):
        return ref[k].astype(jnp.float32)

    projected = sum_over_tp(
        head_block, put_plain, take_plain, head_out, head_in, head_yout, head_yin, head_sem
    )
    middle = normed(
        ALPHA * rows_ref[...].astype(jnp.float32) + projected, gain_ref[...], 0
    ).astype(jnp.bfloat16)
    picked = dot(pick_ref[...], middle).astype(jnp.bfloat16)
    for e in range(ns):
        sbuf[e] = picked[e * pad : e * pad + cap]
    arrivals, notes = [], []
    for hop in range(1, ns):
        to = lax.rem(sp + hop, ns)
        notes.append(
            send(info_ref.at[to], infos.at[sp], info_sem, (hop - 1,), {"sp": to})
        )
        arrivals.append(
            send(sbuf.at[to], gathered.at[tp, sp], sp_sem, (hop - 1,), {"sp": to})
        )
    gathered[tp, sp] = sbuf[sp]
    infos[sp] = info_ref[sp]
    forward, across = [], []
    for hop in range(ns):
        source = lax.rem(sp - hop + ns, ns)
        if hop:
            arrivals[hop - 1].wait_recv()
        mine = gathered.at[tp, source]
        for k in range(1, chips):
            across.append(
                (
                    hop,
                    k,
                    send(
                        mine, mine, y_sem, (hop, k - 1),
                        {"tp": 2 * lax.rem(chip + k, chips) + core},
                    ),
                )
            )
        forward.append(send(mine, mine, pair_sem, (hop, 0), {"tp": partner}))
    for hop, k, copy in across:
        copy.wait_recv()
        source = lax.rem(sp - hop + ns, ns)
        theirs = gathered.at[2 * lax.rem(chip - k + chips, chips) + core, source]
        forward.append(send(theirs, theirs, pair_sem, (hop, k), {"tp": partner}))
    for copy in forward + notes:
        copy.wait_recv()
    for j in range(ns):
        for t in range(nt):
            inputs[j * pad : j * pad + cap, t * width : (t + 1) * width] = gathered[t, j]
        note = columns_of(infos[j])[:pad]
        side[j * pad : (j + 1) * pad] = note
    weight_e, shared_e = side[:, 0:1], side[:, 1:2]
    for load in loads[:4]:
        load.wait()
    shared[...] = (
        jax.nn.silu(dot(inputs[...], cv_ref[...])) * dot(inputs[...], cr_ref[...]) * shared_e
    ).astype(jnp.bfloat16)
    units = hidden.shape[1]
    tile = 256 if units % 256 == 0 else 128

    @pl.loop(0, units // tile)
    def _(i):
        cols = pl.ds(pl.multiple_of(i * tile, tile), tile)
        gate = dot(inputs[...], wv_ref[:, cols])
        up = dot(inputs[...], wr_ref[:, cols])
        hidden[:, cols] = (jax.nn.silu(gate) * up * weight_e).astype(jnp.bfloat16)

    for load in loads[4:]:
        load.wait()

    def part_block(t):
        cols = pl.ds(pl.multiple_of(t * width, width), width)
        return dot(hidden[...], wd_ref[:, cols]) + dot(shared[...], cd_ref[:, cols])

    def put_groups(ref, k, value):
        value = value.astype(ref.dtype)
        for j in range(ns):
            ref[k, j] = value[j * pad : j * pad + cap]

    def take_padded(ref, k):
        for j in range(ns):
            returned[j * pad : j * pad + cap] = ref[k, j]
        return returned[...].astype(jnp.float32)

    summed = sum_over_tp(
        part_block, put_groups, take_padded, part_out, part_in, part_yout, part_yin, part_sem
    )
    put_groups(back_out, 0, summed)
    backs = []
    for hop in range(1, ns):
        to = lax.rem(sp + hop, ns)
        backs.append(send(back_out.at[0, to], back_in.at[sp], back_sem, (hop - 1,), {"sp": to}))
    back_in[sp] = back_out[0, sp]
    for copy in backs:
        copy.wait_recv()
    for j in range(ns):
        returned[j * pad : j * pad + cap] = back_in[j]
    mixture = dot(pick_t_ref[...], returned[...])
    result = normed(ALPHA * middle.astype(jnp.float32) + mixture, last_gain_ref[...], 1)
    out_ref[...] = result.astype(out_ref.dtype)
    for copy in waits:
        copy.wait_send()


def layer(heads_out, wo, rows, gain, last_gain, pick, pick_t, info, weights, cap, pad, cid):
    ns, nt = lax.axis_size("sp"), lax.axis_size("tp")
    chips = nt // 2
    tokens, width = rows.shape
    wv, wr, wd, cv, cr, cd = weights
    half, dma = jnp.bfloat16, pltpu.SemaphoreType.DMA
    across = max(chips - 1, 1)

    def vm(*shape, dtype=half):
        return pltpu.VMEM(shape, dtype)

    scratch = [
        vm(*wv.shape[1:]), vm(*wr.shape[1:]), vm(*wd.shape[1:]),
        vm(*cv.shape), vm(*cr.shape), vm(*cd.shape), dma((6,)),
        vm(chips, tokens, width), vm(chips, tokens, width),
        vm(across, tokens, width), vm(across, tokens, width), dma((2, 2 * chips)),
        vm(2, 8, tokens, dtype=jnp.float32), vm(2, nt - 1, 8, tokens, dtype=jnp.float32),
        dma((2, 2, nt - 1)),
        vm(ns, cap, width), vm(nt, ns, cap, width), vm(ns, 8, 128, dtype=jnp.float32),
        dma((2, ns - 1)), dma((2, ns - 1)), dma((2, ns, across)), dma((2, ns, chips)),
        vm(ns * pad, width * nt), vm(ns * pad, wv.shape[2]), vm(ns * pad, cv.shape[1]),
        vm(ns * pad, 128, dtype=jnp.float32),
        vm(chips, ns, cap, width), vm(chips, ns, cap, width),
        vm(across, ns, cap, width), vm(across, ns, cap, width), dma((2, 2 * chips)),
        vm(1, ns, cap, width), vm(ns, cap, width), dma((2, ns - 1)), vm(ns * pad, width),
    ]
    return pl.pallas_call(
        functools.partial(layer_kernel, ns, nt, cap, pad),
        out_shape=jax.ShapeDtypeStruct((tokens, width), half),
        in_specs=vmem_specs(8) + [pl.BlockSpec(memory_space=pl.ANY)] * 6,
        out_specs=pl.BlockSpec(memory_space=pltpu.VMEM),
        scratch_shapes=scratch,
        compiler_params=pltpu.CompilerParams(
            collective_id=cid, has_side_effects=True, vmem_limit_bytes=60 * 2**20
        ),
        name="layer",
    )(heads_out, wo, rows, gain, last_gain, pick, pick_t, info, *weights)


def block_pass(query_unit, key_unit, write_gate, decay_logarithm, segment, values_in, initial):
    heads_here, blocks, block_len, key_depth = query_unit.shape
    cumulative = jnp.cumsum(decay_logarithm, -1)
    before = jnp.concatenate([segment[:1, 0], segment[:-1, -1]])
    carried = (segment == before[:, None]).astype(jnp.float32)
    same_doc = segment[:, :, None] == segment[:, None, :]
    offsets = jnp.arange(block_len)
    lower_tri = offsets[:, None] >= offsets[None, :]
    strict = offsets[:, None] > offsets[None, :]
    log_gap = cumulative[..., :, None] - cumulative[..., None, :]
    reach_mask = jnp.where(lower_tri & same_doc, jnp.exp(jnp.where(lower_tri, log_gap, 0.0)), 0.0)
    weighted_keys = key_unit * write_gate[..., None]
    coupling = jnp.where(
        strict, matmul_high("hncd,hnsd->hncs", weighted_keys, key_unit) * reach_mask, 0.0
    )
    identity_block = jnp.eye(block_len, dtype=jnp.float32)
    inverse = identity_block - coupling
    nil_power = coupling
    for squaring in range(block_len.bit_length() - 2):
        nil_power = matmul_high("hncs,hnst->hnct", nil_power, nil_power)
        inverse = matmul_high("hncs,hnst->hnct", inverse, identity_block + nil_power)
    growth = jnp.exp(cumulative) * carried
    update = matmul_one("hncs,hnse->hnce", inverse, values_in * write_gate[..., None])
    correction = matmul_one("hncs,hnsd->hncd", inverse, weighted_keys * growth[..., None])
    final_growth = jnp.exp(cumulative[..., -1]) * (segment[:, -1] == before).astype(jnp.float32)
    tail_decay = jnp.exp(cumulative[..., -1:] - cumulative) * (segment == segment[:, -1:]).astype(
        jnp.float32
    )
    tail_keys = key_unit * tail_decay[..., None]
    query_grown = query_unit * growth[..., None]
    local_scores = matmul_one("hncd,hnsd->hncs", query_unit, key_unit) * reach_mask

    def advance(carry_state, inputs):
        grown_query, block_corr, block_update, block_keys, block_scores, block_fade = inputs
        fresh_values = block_update - matmul_one("hcd,hde->hce", block_corr, carry_state)
        next_state = carry_state * block_fade[:, None, None] + matmul_one(
            "hcd,hce->hde", block_keys, fresh_values
        )
        block_out = matmul_one("hcd,hde->hce", grown_query, carry_state) + matmul_one(
            "hcs,hse->hce", block_scores, fresh_values
        )
        return (next_state, block_out)

    inputs = tuple(
        (
            jnp.moveaxis(array, 1, 0)
            for array in (query_grown, correction, update, tail_keys, local_scores, final_growth)
        )
    )
    final_state, outputs = lax.scan(advance, initial, inputs)
    outputs = jnp.moveaxis(outputs, 0, 1).reshape(heads_here, blocks * block_len, -1)
    return (final_state, outputs)


def shards(
    probe_vectors,
    address_vectors,
    content_vectors,
    storage_raw_signal,
    fade_raw_signal,
    channel_fade_exponent,
    extra_fade_amount,
    sequence_label,
    exit_valve_raw_signal,
    final_projection_matrix,
    incoming_rows_matrix,
    initial_rescale_factor,
    specialist_picks,
    picked_specialist_share,
    specialist_valve_matrix,
    specialist_raising_matrix,
    specialist_lowering_matrix,
    common_valve_matrix,
    common_raising_matrix,
    common_lowering_matrix,
    latter_rescale_factor,
):
    tokens_here = probe_vectors.shape[0]
    heads_here = storage_raw_signal.shape[0]
    blocks = tokens_here // BLOCK

    def split_heads(array, width):
        moved = jnp.transpose(
            array.astype(jnp.float32).reshape(tokens_here, heads_here, width), (1, 0, 2)
        )
        return moved.reshape(heads_here, blocks, BLOCK, width)

    query_unit = unit_rows(split_heads(probe_vectors, DK)) * DK ** (-0.5)
    key_unit = unit_rows(split_heads(address_vectors, DK))
    value_rows = split_heads(content_vectors, DV)
    write_gate = jax.nn.sigmoid(storage_raw_signal).reshape(heads_here, blocks, BLOCK)
    decay_logarithm = (
        extra_fade_amount
        - jnp.exp(channel_fade_exponent)[:, None] * jax.nn.softplus(fade_raw_signal)
    ).reshape(heads_here, blocks, BLOCK)
    segment = sequence_label.astype(jnp.float32).reshape(blocks, BLOCK)
    extended = jnp.concatenate(
        [value_rows, jnp.zeros((heads_here, blocks, BLOCK, DK), jnp.float32)], -1
    )
    identity_state = jnp.broadcast_to(jnp.eye(DK, dtype=jnp.float32), (heads_here, DK, DK))
    start_state = jnp.concatenate(
        [jnp.zeros((heads_here, DK, DV), jnp.float32), identity_state], -1
    )
    summary, local_out = block_pass(
        query_unit, key_unit, write_gate, decay_logarithm, segment, extended, start_state
    )
    (edges,) = exchange((sequence_label[None, :],), ("all",), "sp", 0)
    place = lax.axis_index("sp")
    before = lax.dynamic_index_in_dim(edges[:, 0, -1], jnp.maximum(place - 1, 0), 0, False)
    joined = ((before == sequence_label[0]) & (place > 0)).astype(jnp.float32)
    reach = -(-(DOC_SPAN - 1) // tokens_here)
    own = jnp.stack([summary[..., DV:] * joined, summary[..., :DV]]).astype(jnp.bfloat16)
    incoming = entering(own, reach, 1) * joined
    memory_layer_result = local_out[..., :DV] + matmul_one(
        "hcd,hde->hce", local_out[..., DV:], incoming
    )
    scaled = memory_layer_result * lax.rsqrt(
        jnp.mean(memory_layer_result * memory_layer_result, -1, keepdims=True) + 1e-06
    )
    token_major = jnp.transpose(scaled, (1, 0, 2)).reshape(tokens_here, heads_here * DV)
    heads_out = (token_major * jax.nn.silu(exit_valve_raw_signal.astype(jnp.float32))).astype(
        jnp.bfloat16
    )
    top = specialist_picks.shape[1]
    local_experts = specialist_valve_matrix.shape[0]
    experts_all = local_experts * lax.axis_size("sp")
    capacity = max(2, 9 * tokens_here * top // (8 * experts_all))
    picks = tokens_here * top
    flat_routes = specialist_picks.reshape(picks)
    one_hot = (flat_routes[:, None] == jnp.arange(experts_all, dtype=jnp.int32)[None, :]).astype(
        jnp.int32
    )
    rank_in = jnp.sum(jnp.cumsum(one_hot, 0) * one_hot, 1) - 1
    pad = -(-capacity // 16) * 16
    slot_table = (flat_routes * pad + rank_in).reshape(tokens_here, top)
    order = jnp.arange(experts_all * pad, dtype=jnp.int32)
    matches = [order[:, None] == slot_table[None, :, j] for j in range(top)]
    pick = functools.reduce(jnp.logical_or, matches).astype(jnp.bfloat16)
    turned = [order[None, :] == slot_table[:, j, None] for j in range(top)]
    pick_t = functools.reduce(jnp.logical_or, turned).astype(jnp.bfloat16)
    slot_weight = sum(
        jnp.sum(jnp.where(turned[j], picked_specialist_share[:, j, None].astype(jnp.float32), 0.0), 0)
        for j in range(top)
    )
    slot_shared = jnp.any(turned[0], 0).astype(jnp.float32)
    info = jnp.stack([slot_weight, slot_shared]).reshape(2, experts_all, pad)
    info = jnp.pad(jnp.moveaxis(info, 0, 1), ((0, 0), (0, 6), (0, 128 - pad)))
    return layer(
        heads_out,
        final_projection_matrix,
        incoming_rows_matrix,
        initial_rescale_factor[None, :],
        latter_rescale_factor[None, :],
        pick,
        pick_t,
        info,
        (
            specialist_valve_matrix,
            specialist_raising_matrix,
            specialist_lowering_matrix,
            common_valve_matrix,
            common_raising_matrix,
            common_lowering_matrix,
        ),
        capacity,
        pad,
        2,
    )


def solution(mesh):
    placed = (
        P("sp", "tp"),
        P("sp", "tp"),
        P("sp", "tp"),
        P("tp", "sp"),
        P("tp", "sp"),
        P("tp"),
        P("tp", "sp"),
        P("sp"),
        P("sp", "tp"),
        P("tp", None),
        P("sp", "tp"),
        P("tp"),
        P("sp", None),
        P("sp", None),
        P("sp", None, "tp"),
        P("sp", None, "tp"),
        P("sp", "tp", None),
        P(None, "tp"),
        P(None, "tp"),
        P("tp", None),
        P("tp"),
    )
    return jax.shard_map(
        shards, mesh=mesh, in_specs=placed, out_specs=P("sp", "tp"), check_vma=False
    )
```

```python
import functools

import jax
import jax.numpy as jnp
from jax import lax
from jax.experimental import pallas as pl
from jax.experimental.pallas import tpu as pltpu
from jax.sharding import PartitionSpec as P

DK = 128
DV = 128
BLOCK = 64
DOC_SPAN = 768


HIGH = lax.Precision.HIGHEST
ALPHA = 2.0**0.25
MESH = pl.DeviceIdType.MESH


def vmem_specs(count):
    return [pl.BlockSpec(memory_space=pltpu.VMEM)] * count


def scan_plan(n, reach):
    hops = [1]
    covered = 1
    if reach > 1 and n > 2:
        hops.append(2)
        covered = 3
        while covered < min(reach, n - 1):
            hops.append(covered)
            covered = 2 * covered
    return hops


def scan_kernel(n, hops, own_ref, label_ref, out_ref, *scratch):
    rounds = len(hops)
    landed, built = scratch[:rounds], scratch[rounds : 2 * rounds]
    send_sem, recv_sem, label_in, label_sem = scratch[2 * rounds :]
    heads = own_ref.shape[1]
    me = lax.axis_index("sp")
    barrier = pltpu.get_barrier_semaphore()
    for hop in range(1, n):
        pl.semaphore_signal(
            barrier, inc=1, device_id={"sp": lax.rem(me + hop, n)}, device_id_type=MESH
        )
    pl.semaphore_wait(barrier, n - 1)

    def dot(left, right):
        return jnp.dot(left, right, preferred_element_type=jnp.float32)

    def copy_of(index):
        last = index == rounds - 1 and index > 1
        source = built[index]
        landing = landed[index]
        if last:
            source, landing = source.at[1], landing.at[1]
        return pltpu.make_async_remote_copy(
            src_ref=source,
            dst_ref=landing,
            send_sem=send_sem.at[index],
            recv_sem=recv_sem.at[index],
            device_id={"sp": lax.rem(me + hops[index], n)},
            device_id_type=MESH,
        )

    note = pltpu.make_async_remote_copy(
        src_ref=label_ref,
        dst_ref=label_in,
        send_sem=label_sem.at[0],
        recv_sem=label_sem.at[1],
        device_id={"sp": lax.rem(me + 1, n)},
        device_id_type=MESH,
    )
    note.start()
    note.wait_recv()
    before, first = label_in[0:1, label_in.shape[1] - 1 :], label_ref[0:1, 0:1]
    joined = ((before == first) & (me > 0)).astype(jnp.float32)
    for h in range(heads):
        built[0][0, h] = (own_ref[0, h] * joined).astype(built[0].dtype)
        built[0][1, h] = own_ref[1, h].astype(built[0].dtype)
    window = None
    for index, hop in enumerate(hops):
        copy = copy_of(index)
        last = index == rounds - 1

        @pl.when(me + hop < n)
        def _():
            copy.start()

        @pl.when(me >= hop)
        def _():
            copy.wait_recv()

        @pl.when(me < hop)
        def _():
            landed[index][...] = jnp.zeros_like(landed[index])

        got = landed[index]
        if index == 0:
            if last:
                out_ref[...] = got[1].astype(jnp.float32) * joined
            else:
                later, target = built[0], built[1]
                for h in range(heads):
                    target[0, h] = dot(later[0, h], got[0, h]).astype(target.dtype)
                    target[1, h] = (
                        dot(later[0, h], got[1, h]) + later[1, h].astype(jnp.float32)
                    ).astype(target.dtype)
            window = got
        else:
            for h in range(heads):
                shift = dot(window[0, h], got[1, h]) + window[1, h].astype(jnp.float32)
                if last:
                    out_ref[h] = shift * joined
                else:
                    target = built[index + 1]
                    target[0, h] = dot(window[0, h], got[0, h]).astype(target.dtype)
                    target[1, h] = shift.astype(target.dtype)
            if not last:
                window = built[index + 1]
    for index, hop in enumerate(hops):

        @pl.when(me + hop < n)
        def _():
            copy_of(index).wait_send()

    note.wait_send()


def entering(summary, labels, reach, cid):
    n = lax.axis_size("sp")
    hops = scan_plan(n, reach)
    block = pltpu.VMEM(summary.shape, jnp.bfloat16)
    return pl.pallas_call(
        functools.partial(scan_kernel, n, hops),
        out_shape=jax.ShapeDtypeStruct(summary.shape[1:], jnp.float32),
        in_specs=vmem_specs(2),
        out_specs=pl.BlockSpec(memory_space=pltpu.VMEM),
        scratch_shapes=[block] * (2 * len(hops))
        + [pltpu.SemaphoreType.DMA((len(hops),)), pltpu.SemaphoreType.DMA((len(hops),))]
        + [pltpu.VMEM(labels.shape, labels.dtype), pltpu.SemaphoreType.DMA((2,))],
        compiler_params=pltpu.CompilerParams(collective_id=cid, has_side_effects=True),
        name="state_scan",
    )(summary, labels)


def unit_rows(array):
    return array * lax.rsqrt(jnp.sum(array * array, -1, keepdims=True) + 1e-06)


def matmul_high(form, left, right):
    return jnp.einsum(form, left, right, precision=HIGH)


def matmul_one(form, left, right):
    return jnp.einsum(
        form,
        left.astype(jnp.bfloat16),
        right.astype(jnp.bfloat16),
        preferred_element_type=jnp.float32,
    )


def row_stats(array):
    lane = lax.broadcasted_iota(jnp.int32, (array.shape[0], 128), 1)
    total = jnp.sum(array, -1, keepdims=True)
    square = jnp.sum(array * array, -1, keepdims=True)
    return jnp.where(lane == 0, total, jnp.where(lane == 1, square, 0.0)).T[:8]


def columns_of(rows):
    return jnp.concatenate([rows] * (128 // rows.shape[0]), 0).T


def layer_kernel(
    ns, nt, cap, pad, heads_ref, wo_ref, rows_ref, gain_ref, last_gain_ref, pick_ref, pick_t_ref,
    info_ref, wv_hbm, wr_hbm, wd_hbm, cv_hbm, cr_hbm, cd_hbm, out_ref,
    wv_ref, wr_ref, wd_ref, cv_ref, cr_ref, cd_ref, weight_sem,
    head_out, head_in, head_yout, head_yin, head_sem,
    stat_own, stat_in, stat_sem,
    sbuf, gathered, infos, sp_sem, info_sem, y_sem, pair_sem,
    inputs, hidden, shared, side, part_out, part_in, part_yout, part_yin, part_sem,
    back_out, back_in, back_sem, returned,
):
    sp, tp = lax.axis_index("sp"), lax.axis_index("tp")
    chips = nt // 2
    chip, core = tp // 2, lax.rem(tp, 2)
    partner = tp + 1 - 2 * core
    width = out_ref.shape[-1]
    loads = [
        pltpu.make_async_copy(source, target, weight_sem.at[i])
        for i, (source, target) in enumerate(
            (
                (cv_hbm, cv_ref),
                (cr_hbm, cr_ref),
                (wv_hbm.at[0], wv_ref),
                (wr_hbm.at[0], wr_ref),
                (cd_hbm, cd_ref),
                (wd_hbm.at[0], wd_ref),
            )
        )
    ]
    for load in loads:
        load.start()
    barrier = pltpu.get_barrier_semaphore()
    for hop in range(1, ns):
        pl.semaphore_signal(
            barrier, inc=1, device_id={"sp": lax.rem(sp + hop, ns)}, device_id_type=MESH
        )
    for hop in range(1, nt):
        pl.semaphore_signal(
            barrier, inc=1, device_id={"tp": lax.rem(tp + hop, nt)}, device_id_type=MESH
        )
    inputs[...] = jnp.zeros_like(inputs)
    returned[...] = jnp.zeros_like(returned)
    pl.semaphore_wait(barrier, ns - 1 + nt - 1)
    waits = []

    def send(source, target, sems, place, where):
        copy = pltpu.make_async_remote_copy(
            src_ref=source,
            dst_ref=target,
            send_sem=sems.at[(0,) + place],
            recv_sem=sems.at[(1,) + place],
            device_id=where,
            device_id_type=MESH,
        )
        copy.start()
        waits.append(copy)
        return copy

    def dot(left, right):
        return jnp.dot(left, right, preferred_element_type=jnp.float32)

    def sum_over_tp(block, put, take, out, landed, yout, yin, sems):
        order = list(range(1, chips)) + [0]
        pairs = {}
        for k in order:
            put(out, k, block(2 * lax.rem(chip + k, chips) + 1 - core))
            pairs[k] = send(out.at[k], landed.at[k], sems, (k,), {"tp": partner})
        across = []
        for k in order:
            there = 2 * lax.rem(chip + k, chips) + core
            value = block(there)
            pairs[k].wait_recv()
            value = value + take(landed, k)
            if k:
                put(yout, k - 1, value)
                across.append(
                    send(yout.at[k - 1], yin.at[k - 1], sems, (chips + k - 1,), {"tp": there})
                )
        for k, copy in enumerate(across):
            copy.wait_recv()
            value = value + take(yin, k)
        return value

    def normed(summed, gain, index):
        stat_own[index] = row_stats(summed)
        copies = []
        for hop in range(1, nt):
            copies.append(
                send(
                    stat_own.at[index],
                    stat_in.at[index, hop - 1],
                    stat_sem,
                    (index, hop - 1),
                    {"tp": lax.rem(tp + hop, nt)},
                )
            )
        total = stat_own[index]
        for hop in range(1, nt):
            copies[hop - 1].wait_recv()
            total = total + stat_in[index, hop - 1]
        total = columns_of(total / (width * nt))
        mean, square = total[:, 0:1], total[:, 1:2]
        return (summed - mean) * lax.rsqrt(square - mean * mean + 1e-05) * gain

    def head_block(t):
        start = pl.multiple_of(t * width, width)
        return dot(heads_ref[...], wo_ref[:, pl.ds(start, width)])

    def put_plain(ref, k, value):
        ref[k] = value.astype(ref.dtype)

    def take_plain(ref, k):
        return ref[k].astype(jnp.float32)

    projected = sum_over_tp(
        head_block, put_plain, take_plain, head_out, head_in, head_yout, head_yin, head_sem
    )
    middle = normed(
        ALPHA * rows_ref[...].astype(jnp.float32) + projected, gain_ref[...], 0
    ).astype(jnp.bfloat16)
    picked = dot(pick_ref[...], middle).astype(jnp.bfloat16)
    for e in range(ns):
        sbuf[e] = picked[e * pad : e * pad + cap]
    arrivals, notes = [], []
    for hop in range(1, ns):
        to = lax.rem(sp + hop, ns)
        notes.append(
            send(info_ref.at[to], infos.at[sp], info_sem, (hop - 1,), {"sp": to})
        )
        arrivals.append(
            send(sbuf.at[to], gathered.at[tp, sp], sp_sem, (hop - 1,), {"sp": to})
        )
    gathered[tp, sp] = sbuf[sp]
    infos[sp] = info_ref[sp]
    forward, across = [], []
    for hop in range(ns):
        source = lax.rem(sp - hop + ns, ns)
        if hop:
            arrivals[hop - 1].wait_recv()
        mine = gathered.at[tp, source]
        for k in range(1, chips):
            across.append(
                (
                    hop,
                    k,
                    send(
                        mine, mine, y_sem, (hop, k - 1),
                        {"tp": 2 * lax.rem(chip + k, chips) + core},
                    ),
                )
            )
        forward.append(send(mine, mine, pair_sem, (hop, 0), {"tp": partner}))
    for hop, k, copy in across:
        copy.wait_recv()
        source = lax.rem(sp - hop + ns, ns)
        theirs = gathered.at[2 * lax.rem(chip - k + chips, chips) + core, source]
        forward.append(send(theirs, theirs, pair_sem, (hop, k), {"tp": partner}))
    for copy in forward + notes:
        copy.wait_recv()
    for j in range(ns):
        for t in range(nt):
            inputs[j * pad : j * pad + cap, t * width : (t + 1) * width] = gathered[t, j]
        note = columns_of(infos[j])[:pad]
        side[j * pad : (j + 1) * pad] = note
    weight_e, shared_e = side[:, 0:1], side[:, 1:2]
    for load in loads[:4]:
        load.wait()
    shared[...] = (
        jax.nn.silu(dot(inputs[...], cv_ref[...])) * dot(inputs[...], cr_ref[...]) * shared_e
    ).astype(jnp.bfloat16)
    units = hidden.shape[1]
    tile = 256 if units % 256 == 0 else 128

    @pl.loop(0, units // tile)
    def _(i):
        cols = pl.ds(pl.multiple_of(i * tile, tile), tile)
        gate = dot(inputs[...], wv_ref[:, cols])
        up = dot(inputs[...], wr_ref[:, cols])
        hidden[:, cols] = (jax.nn.silu(gate) * up * weight_e).astype(jnp.bfloat16)

    for load in loads[4:]:
        load.wait()

    def part_block(t):
        cols = pl.ds(pl.multiple_of(t * width, width), width)
        return dot(hidden[...], wd_ref[:, cols]) + dot(shared[...], cd_ref[:, cols])

    def put_groups(ref, k, value):
        value = value.astype(ref.dtype)
        for j in range(ns):
            ref[k, j] = value[j * pad : j * pad + cap]

    def take_padded(ref, k):
        for j in range(ns):
            returned[j * pad : j * pad + cap] = ref[k, j]
        return returned[...].astype(jnp.float32)

    summed = sum_over_tp(
        part_block, put_groups, take_padded, part_out, part_in, part_yout, part_yin, part_sem
    )
    put_groups(back_out, 0, summed)
    backs = []
    for hop in range(1, ns):
        to = lax.rem(sp + hop, ns)
        backs.append(send(back_out.at[0, to], back_in.at[sp], back_sem, (hop - 1,), {"sp": to}))
    back_in[sp] = back_out[0, sp]
    for copy in backs:
        copy.wait_recv()
    for j in range(ns):
        returned[j * pad : j * pad + cap] = back_in[j]
    mixture = dot(pick_t_ref[...], returned[...])
    result = normed(ALPHA * middle.astype(jnp.float32) + mixture, last_gain_ref[...], 1)
    out_ref[...] = result.astype(out_ref.dtype)
    for copy in waits:
        copy.wait_send()


def layer(heads_out, wo, rows, gain, last_gain, pick, pick_t, info, weights, cap, pad, cid):
    ns, nt = lax.axis_size("sp"), lax.axis_size("tp")
    chips = nt // 2
    tokens, width = rows.shape
    wv, wr, wd, cv, cr, cd = weights
    half, dma = jnp.bfloat16, pltpu.SemaphoreType.DMA
    across = max(chips - 1, 1)

    def vm(*shape, dtype=half):
        return pltpu.VMEM(shape, dtype)

    scratch = [
        vm(*wv.shape[1:]), vm(*wr.shape[1:]), vm(*wd.shape[1:]),
        vm(*cv.shape), vm(*cr.shape), vm(*cd.shape), dma((6,)),
        vm(chips, tokens, width), vm(chips, tokens, width),
        vm(across, tokens, width), vm(across, tokens, width), dma((2, 2 * chips)),
        vm(2, 8, tokens, dtype=jnp.float32), vm(2, nt - 1, 8, tokens, dtype=jnp.float32),
        dma((2, 2, nt - 1)),
        vm(ns, cap, width), vm(nt, ns, cap, width), vm(ns, 8, 128, dtype=jnp.float32),
        dma((2, ns - 1)), dma((2, ns - 1)), dma((2, ns, across)), dma((2, ns, chips)),
        vm(ns * pad, width * nt), vm(ns * pad, wv.shape[2]), vm(ns * pad, cv.shape[1]),
        vm(ns * pad, 128, dtype=jnp.float32),
        vm(chips, ns, cap, width), vm(chips, ns, cap, width),
        vm(across, ns, cap, width), vm(across, ns, cap, width), dma((2, 2 * chips)),
        vm(1, ns, cap, width), vm(ns, cap, width), dma((2, ns - 1)), vm(ns * pad, width),
    ]
    return pl.pallas_call(
        functools.partial(layer_kernel, ns, nt, cap, pad),
        out_shape=jax.ShapeDtypeStruct((tokens, width), half),
        in_specs=vmem_specs(8) + [pl.BlockSpec(memory_space=pl.ANY)] * 6,
        out_specs=pl.BlockSpec(memory_space=pltpu.VMEM),
        scratch_shapes=scratch,
        compiler_params=pltpu.CompilerParams(
            collective_id=cid, has_side_effects=True, vmem_limit_bytes=60 * 2**20
        ),
        name="layer",
    )(heads_out, wo, rows, gain, last_gain, pick, pick_t, info, *weights)


def block_pass(query_unit, key_unit, write_gate, decay_logarithm, segment, values_in, initial):
    heads_here, blocks, block_len, key_depth = query_unit.shape
    cumulative = jnp.cumsum(decay_logarithm, -1)
    before = jnp.concatenate([segment[:1, 0], segment[:-1, -1]])
    carried = (segment == before[:, None]).astype(jnp.float32)
    same_doc = segment[:, :, None] == segment[:, None, :]
    offsets = jnp.arange(block_len)
    lower_tri = offsets[:, None] >= offsets[None, :]
    strict = offsets[:, None] > offsets[None, :]
    log_gap = cumulative[..., :, None] - cumulative[..., None, :]
    reach_mask = jnp.where(lower_tri & same_doc, jnp.exp(jnp.where(lower_tri, log_gap, 0.0)), 0.0)
    weighted_keys = key_unit * write_gate[..., None]
    coupling = jnp.where(
        strict, matmul_high("hncd,hnsd->hncs", weighted_keys, key_unit) * reach_mask, 0.0
    )
    identity_block = jnp.eye(block_len, dtype=jnp.float32)
    inverse = identity_block - coupling
    nil_power = coupling
    for squaring in range(block_len.bit_length() - 2):
        nil_power = matmul_high("hncs,hnst->hnct", nil_power, nil_power)
        inverse = matmul_high("hncs,hnst->hnct", inverse, identity_block + nil_power)
    growth = jnp.exp(cumulative) * carried
    update = matmul_one("hncs,hnse->hnce", inverse, values_in * write_gate[..., None])
    correction = matmul_one("hncs,hnsd->hncd", inverse, weighted_keys * growth[..., None])
    final_growth = jnp.exp(cumulative[..., -1]) * (segment[:, -1] == before).astype(jnp.float32)
    tail_decay = jnp.exp(cumulative[..., -1:] - cumulative) * (segment == segment[:, -1:]).astype(
        jnp.float32
    )
    tail_keys = key_unit * tail_decay[..., None]
    query_grown = query_unit * growth[..., None]
    local_scores = matmul_one("hncd,hnsd->hncs", query_unit, key_unit) * reach_mask

    def advance(carry_state, inputs):
        grown_query, block_corr, block_update, block_keys, block_scores, block_fade = inputs
        fresh_values = block_update - matmul_one("hcd,hde->hce", block_corr, carry_state)
        next_state = carry_state * block_fade[:, None, None] + matmul_one(
            "hcd,hce->hde", block_keys, fresh_values
        )
        block_out = matmul_one("hcd,hde->hce", grown_query, carry_state) + matmul_one(
            "hcs,hse->hce", block_scores, fresh_values
        )
        return (next_state, block_out)

    inputs = tuple(
        (
            jnp.moveaxis(array, 1, 0)
            for array in (query_grown, correction, update, tail_keys, local_scores, final_growth)
        )
    )
    final_state, outputs = lax.scan(advance, initial, inputs)
    outputs = jnp.moveaxis(outputs, 0, 1).reshape(heads_here, blocks * block_len, -1)
    return (final_state, outputs)


def shards(
    probe_vectors,
    address_vectors,
    content_vectors,
    storage_raw_signal,
    fade_raw_signal,
    channel_fade_exponent,
    extra_fade_amount,
    sequence_label,
    exit_valve_raw_signal,
    final_projection_matrix,
    incoming_rows_matrix,
    initial_rescale_factor,
    specialist_picks,
    picked_specialist_share,
    specialist_valve_matrix,
    specialist_raising_matrix,
    specialist_lowering_matrix,
    common_valve_matrix,
    common_raising_matrix,
    common_lowering_matrix,
    latter_rescale_factor,
):
    tokens_here = probe_vectors.shape[0]
    heads_here = storage_raw_signal.shape[0]
    blocks = tokens_here // BLOCK

    def split_heads(array, width):
        moved = jnp.transpose(
            array.astype(jnp.float32).reshape(tokens_here, heads_here, width), (1, 0, 2)
        )
        return moved.reshape(heads_here, blocks, BLOCK, width)

    query_unit = unit_rows(split_heads(probe_vectors, DK)) * DK ** (-0.5)
    key_unit = unit_rows(split_heads(address_vectors, DK))
    value_rows = split_heads(content_vectors, DV)
    write_gate = jax.nn.sigmoid(storage_raw_signal).reshape(heads_here, blocks, BLOCK)
    decay_logarithm = (
        extra_fade_amount
        - jnp.exp(channel_fade_exponent)[:, None] * jax.nn.softplus(fade_raw_signal)
    ).reshape(heads_here, blocks, BLOCK)
    segment = sequence_label.astype(jnp.float32).reshape(blocks, BLOCK)
    extended = jnp.concatenate(
        [value_rows, jnp.zeros((heads_here, blocks, BLOCK, DK), jnp.float32)], -1
    )
    identity_state = jnp.broadcast_to(jnp.eye(DK, dtype=jnp.float32), (heads_here, DK, DK))
    start_state = jnp.concatenate(
        [jnp.zeros((heads_here, DK, DV), jnp.float32), identity_state], -1
    )
    summary, local_out = block_pass(
        query_unit, key_unit, write_gate, decay_logarithm, segment, extended, start_state
    )
    reach = -(-(DOC_SPAN - 1) // tokens_here)
    own = jnp.stack([summary[..., DV:], summary[..., :DV]])
    incoming = entering(own, sequence_label[None, :], reach, 1)
    memory_layer_result = local_out[..., :DV] + matmul_one(
        "hcd,hde->hce", local_out[..., DV:], incoming
    )
    scaled = memory_layer_result * lax.rsqrt(
        jnp.mean(memory_layer_result * memory_layer_result, -1, keepdims=True) + 1e-06
    )
    token_major = jnp.transpose(scaled, (1, 0, 2)).reshape(tokens_here, heads_here * DV)
    heads_out = (token_major * jax.nn.silu(exit_valve_raw_signal.astype(jnp.float32))).astype(
        jnp.bfloat16
    )
    top = specialist_picks.shape[1]
    local_experts = specialist_valve_matrix.shape[0]
    experts_all = local_experts * lax.axis_size("sp")
    capacity = max(2, 9 * tokens_here * top // (8 * experts_all))
    picks = tokens_here * top
    flat_routes = specialist_picks.reshape(picks)
    one_hot = (flat_routes[:, None] == jnp.arange(experts_all, dtype=jnp.int32)[None, :]).astype(
        jnp.int32
    )
    rank_in = jnp.sum(jnp.cumsum(one_hot, 0) * one_hot, 1) - 1
    pad = -(-capacity // 16) * 16
    slot_table = (flat_routes * pad + rank_in).reshape(tokens_here, top)
    order = jnp.arange(experts_all * pad, dtype=jnp.int32)
    matches = [order[:, None] == slot_table[None, :, j] for j in range(top)]
    pick = functools.reduce(jnp.logical_or, matches).astype(jnp.bfloat16)
    turned = [order[None, :] == slot_table[:, j, None] for j in range(top)]
    pick_t = functools.reduce(jnp.logical_or, turned).astype(jnp.bfloat16)
    slot_weight = sum(
        jnp.sum(jnp.where(turned[j], picked_specialist_share[:, j, None].astype(jnp.float32), 0.0), 0)
        for j in range(top)
    )
    slot_shared = jnp.any(turned[0], 0).astype(jnp.float32)
    info = jnp.stack([slot_weight, slot_shared]).reshape(2, experts_all, pad)
    info = jnp.pad(jnp.moveaxis(info, 0, 1), ((0, 0), (0, 6), (0, 128 - pad)))
    return layer(
        heads_out,
        final_projection_matrix,
        incoming_rows_matrix,
        initial_rescale_factor[None, :],
        latter_rescale_factor[None, :],
        pick,
        pick_t,
        info,
        (
            specialist_valve_matrix,
            specialist_raising_matrix,
            specialist_lowering_matrix,
            common_valve_matrix,
            common_raising_matrix,
            common_lowering_matrix,
        ),
        capacity,
        pad,
        2,
    )


def solution(mesh):
    placed = (
        P("sp", "tp"),
        P("sp", "tp"),
        P("sp", "tp"),
        P("tp", "sp"),
        P("tp", "sp"),
        P("tp"),
        P("tp", "sp"),
        P("sp"),
        P("sp", "tp"),
        P("tp", None),
        P("sp", "tp"),
        P("tp"),
        P("sp", None),
        P("sp", None),
        P("sp", None, "tp"),
        P("sp", None, "tp"),
        P("sp", "tp", None),
        P(None, "tp"),
        P(None, "tp"),
        P("tp", None),
        P("tp"),
    )
    return jax.shard_map(
        shards, mesh=mesh, in_specs=placed, out_specs=P("sp", "tp"), check_vma=False
    )
```
